128 devices in a mesh: grp: 4 (over y, x), ep: 32 (over z, core).
Axes of the slice: x: 2, y: 2, z: 16, core: 2. Of those that a mesh axis runs over, the one named last changes fastest.
The devices are a block of a 8x8x16 slice.
Arguments:
- tokens: bfloat16 [32768, 2048], P(('grp', 'ep')), parts along dimension 0, may hold values from -6 to 6
- norm_gain: float32 [2048], replicated, may hold values from 0.1 to 1.9
- expert_ids: int32 [32768, 2], P(('grp', 'ep')), parts along dimension 0, may hold values from 0 to 31, all different within a row; in each aligned block of 256 rows (0 to 255, 256 to 511, ...) at most 32 rows name the same one
- gate_weights: float32 [32768, 2], P(('grp', 'ep')), parts along dimension 0, may hold values from 0.1 to 1
- w_gate: bfloat16 [32, 2048, 1024], P('ep'), may hold values from -0.125 to 0.125
- w_up: bfloat16 [32, 2048, 1024], P('ep'), may hold values from -0.125 to 0.125
- w_down: bfloat16 [32, 1024, 2048], P('ep'), may hold values from -0.1875 to 0.1875
Outputs:
- mixed: bfloat16 [32768, 2048], P(('grp', 'ep')), parts along dimension 0
The draws below stay inside these ranges and needn't reach their ends.
There are 4 independent parts, one for each index of `grp`. The reference program is written for one: setup_inputs(seed, part) draws one part's arguments, and reference() takes and returns one part's arrays. A program takes and returns all parts, laid end to end along the dimension named above; an argument that names none is the same for every part. Nothing has to cross between parts.
Inputs may be any that keep to these rules, and one draw needn't show every extreme that they name: `expert_ids`: A token's 2 experts are distinct. Within the rows of one device (aligned blocks of 256 tokens) no expert is named more than 32 times, and in some block one expert is named exactly 32 times.
All inputs are finite; a program needn't handle non-finite values.
Results may differ from the reference program's by a relative error of at most 0.0071.
Values may be sent and summed in bfloat16 or wider, within the bound.
No kernel may reach another device: no remote copies, remote signals or barrier semaphores. Data moves between devices by JAX's collectives and lax.ppermute only.
A program may use at most 64 MiB of HBM per device.

```python
import math
import jax
import jax.numpy as jnp
import numpy as np
from jax import lax

D = 2048
FF = 1024
TOP = 2
TOK_DEV = 256
EXPERTS = 32
CAP = 32
TOKENS = 8192
N_EP = 32


def steps_of(stream_key, extent, shards, smallest, high):
    def one(axis_at, shards_of):
        draws = jax.random.uniform(jax.random.fold_in(jax.random.fold_in(stream_key, 6), axis_at), (shards_of,), jnp.float32, smallest / len(shards), high / len(shards))
        return jnp.repeat(jnp.exp(draws), extent[axis_at] // shards_of).reshape((-1,) + (1,) * (len(extent) - axis_at - 1))

    level = one(*shards[0])
    for cut in shards[1:]:
        level = level * one(*cut)
    return level


def shared_out(own_key, own, number, rows, amount, top, bound, lean):
    ranking = jax.random.permutation(own_key, amount)
    heavy_load, common = shares(amount, rows * top, bound, lean, True), shares(amount, rows * top, bound, lean, False)
    places = jnp.arange(amount)

    def named(lengths, rotation):
        used = int((lengths > 0).sum())
        fixed = max(1, used // 4)
        shifted = fixed + (places - fixed + rotation * (used - fixed)) % max(1, amount - fixed)
        return jnp.zeros((amount,), jnp.int32).at[ranking[jnp.where(places < fixed, places, shifted)]].set(jnp.asarray(lengths, jnp.int32))

    lengths = jnp.where(number % 4 == 0, named(heavy_load, number // 4), named(common, number - number // 4 - 1))
    mixed = jax.random.permutation(jax.random.fold_in(own, 3), amount)
    giver, taker = mixed[0:amount // 2 * 2:2], mixed[1:amount // 2 * 2:2]
    margin = jnp.minimum(lengths[giver] - 1, bound - lengths[taker]) // 2
    margin = jnp.where((giver == ranking[0]) | (taker == ranking[0]) | (lengths[taker] == 0), 0, jnp.maximum(margin, 0))
    shifted = jax.random.randint(jax.random.fold_in(own, 4), (amount // 2,), 0, 1 << 20) % (margin + 1)
    lengths = lengths.at[giver].add(-shifted).at[taker].add(shifted)
    members = jnp.searchsorted(jnp.cumsum(lengths), jnp.arange(rows * top), side="right").astype(jnp.int32)
    listing = members.reshape(top, rows).T
    listing = listing[jax.random.permutation(jax.random.fold_in(own, 1), rows)]
    rotation = jax.random.randint(jax.random.fold_in(own, 2), (rows, 1), 0, top)
    return jnp.take_along_axis(listing, (jnp.arange(top)[None, :] + rotation) % top, axis=1)


def shares(count, total, most, skew, full):
    loads = [(1 << 20) // math.isqrt(rank ** skew) + 1 for rank in range(1, count + 1)]
    largest = most if full else min(most, max(-(-total // count), total * loads[0] // sum(loads)))
    least = 1 if total - largest >= count - 1 else 0
    holding, spare = [largest] + [least] * (count - 1), total - largest - least * (count - 1)
    while spare > 0:
        movable = [i for i in range(1, count) if holding[i] < largest] or [i for i in range(1, count) if holding[i] < most]
        mass, remaining = sum([loads[i] for i in movable]), spare
        for i in movable:
            extra = min(most - holding[i], max(1, remaining * loads[i] // mass), spare)
            holding[i] = holding[i] + extra
            spare = spare - extra
    return np.array(holding)


def centred(stream_key, shape, width, reach, split=(), kind=jnp.bfloat16):
    drawn = width * jax.random.normal(stream_key, shape, jnp.float32)
    if split:
        drawn = drawn * steps_of(stream_key, shape, split, -0.22, 0.18)
    return jnp.clip(drawn, -reach, reach).astype(kind)


def setup_inputs(seed: int = 0, part: int = 0) -> dict:
    key_list = jax.random.split(jax.random.key(seed), 8)
    part_splits = jax.random.split(jax.random.fold_in(key_list[7], part), 8)
    tokens = centred(part_splits[0], (TOKENS, D), 1.0, 6.0, ((0, 32),))
    norm_gain = jnp.clip(1.0 + 0.18 * jax.random.normal(key_list[1], (D,), jnp.float32), 0.1, 1.9)
    expert_ids_keys = jax.random.split(jax.random.fold_in(part_splits[2], 1), TOKENS // TOK_DEV)
    expert_ids_turns = jax.random.permutation(jax.random.fold_in(part_splits[2], 3), TOKENS // TOK_DEV)
    expert_ids = jax.vmap(lambda own, number: shared_out(jax.random.fold_in(part_splits[2], 2), own, number, TOK_DEV, EXPERTS, TOP, CAP, 2))(expert_ids_keys, expert_ids_turns).reshape((TOKENS, TOP))
    gate_weights = jnp.clip(0.1 + 0.9 * jax.random.uniform(part_splits[3], (TOKENS, TOP), jnp.float32) ** steps_of(part_splits[3], (TOKENS, TOP), ((0, 32),), -0.2, 0.2), 0.1, 1.0)
    w_gate = centred(key_list[4], (EXPERTS, D, FF), D ** -0.5, 0.125, ((0, 32),))
    w_up = centred(key_list[5], (EXPERTS, D, FF), D ** -0.5, 0.125, ((0, 32),))
    w_down = centred(key_list[6], (EXPERTS, FF, D), FF ** -0.5, 0.1875, ((0, 32),))
    return dict(tokens=tokens, norm_gain=norm_gain, expert_ids=expert_ids, gate_weights=gate_weights, w_gate=w_gate, w_up=w_up, w_down=w_down)


def reference(tokens, norm_gain, expert_ids, gate_weights, w_gate, w_up, w_down):
    values = tokens.astype(jnp.float32)
    normed = (values * lax.rsqrt(lax.optimization_barrier(jnp.mean(values * values, -1, keepdims=True)) + 1e-06) * norm_gain).astype(jnp.bfloat16)
    flat_ids = expert_ids.reshape(N_EP, TOK_DEV * TOP)
    onehot = (flat_ids[:, :, None] == jnp.arange(EXPERTS, dtype=jnp.int32)[None, None, :]).astype(jnp.int32)
    before = jnp.cumsum(onehot, axis=1) - onehot
    slots = lax.optimization_barrier(jnp.sum(onehot * before, axis=-1)).astype(jnp.int32)
    dest = (flat_ids * CAP + slots).astype(jnp.int32)
    copies = jnp.repeat(normed.reshape(N_EP, TOK_DEV, D), TOP, axis=1)
    buffers = jnp.zeros((N_EP, EXPERTS * CAP, D), jnp.bfloat16)
    sources = jnp.arange(N_EP, dtype=jnp.int32)[:, None]
    buffers = buffers.at[sources, dest].set(copies)
    buffers = buffers.reshape(N_EP, EXPERTS, CAP, D).transpose(1, 0, 2, 3).reshape(EXPERTS, N_EP * CAP, D)

    def run(operands):
        rows, gate_w, up_w, down_w = operands
        gate = jnp.dot(rows, gate_w, preferred_element_type=jnp.float32)
        upper = jnp.dot(rows, up_w, preferred_element_type=jnp.float32)
        hidden = (jax.nn.silu(gate) * upper).astype(jnp.bfloat16)
        return jnp.dot(hidden, down_w, preferred_element_type=jnp.float32).astype(jnp.bfloat16)
    results = lax.map(run, (buffers, w_gate, w_up, w_down))
    results = results.reshape(EXPERTS, N_EP, CAP, D).transpose(1, 0, 2, 3).reshape(N_EP, EXPERTS * CAP, D)
    back = jnp.take_along_axis(results, dest[:, :, None], axis=1).astype(jnp.float32)
    back = back.reshape(N_EP, TOK_DEV, TOP, D)
    weights = gate_weights.reshape(N_EP, TOK_DEV, TOP)
    mixed = lax.optimization_barrier(jnp.sum(back * weights[:, :, :, None], axis=2))
    return mixed.reshape(TOKENS, D).astype(jnp.bfloat16)
```

```python
import jax
import jax.numpy as jnp
from jax import lax
from jax.sharding import PartitionSpec as P

BF = jnp.bfloat16
F32 = jnp.float32
HALVES = 2


def dot(a, b, dims=((1,), (0,))):
    return lax.dot_general(a, b, (dims, ((), ())), preferred_element_type=F32)


def per_device(tokens, norm_gain, expert_ids, gate_weights, w_gate, w_up, w_down):
    ep = lax.axis_size("ep")
    chips = ep // 2
    far = chips // 2
    rows, width = tokens.shape
    cap = 2 * rows * expert_ids.shape[1] // ep
    size = {t: min(rows, cap * (2 * (far - t) + 1)) for t in range(1, far + 1)}
    near = max(t for t in size if size[t] == rows)
    part = width // HALVES
    me = lax.axis_index("ep")
    chip, core = me // 2, me % 2

    def shift(x, hops):
        return lax.ppermute(x, "ep", [(i, (i + 2 * hops) % ep) for i in range(ep)])

    def swap(x):
        return lax.ppermute(x, "ep", [(i, i ^ 1) for i in range(ep)])

    values = tokens.astype(F32)
    scale = lax.rsqrt(jnp.mean(values * values, -1) + 1e-06)
    code = (expert_ids[:, 0] * ep + expert_ids[:, 1]).astype(F32)
    meta = jnp.stack([code, gate_weights[:, 0], gate_weights[:, 1], scale])
    order = [0]
    for t in range(1, far):
        order += [t, -t]
    order.append(far)
    where = {d: i for i, d in enumerate(order)}
    metas = jnp.stack([meta if d == 0 else shift(meta, d) for d in order])
    codes = metas[:, 0].astype(jnp.int32)
    first, second = codes // ep, codes % ep
    experts = jnp.stack([me, me ^ 1])[None, :, None]
    hit1 = first[:, None, :] == experts
    hit2 = second[:, None, :] == experts
    hit = hit1 | hit2
    weight = jnp.where(hit1, metas[:, None, 1], 0.0) + jnp.where(hit2, metas[:, None, 2], 0.0)
    before = (
        lax.broadcasted_iota(jnp.int32, (rows, rows), 0)
        < lax.broadcasted_iota(jnp.int32, (rows, rows), 1)
    ).astype(BF)
    slot = dot(hit.astype(BF).reshape(-1, rows), before).reshape(hit.shape)
    picks = hit[:, :, None, :] & (
        slot[:, :, None, :] == jnp.arange(cap, dtype=F32)[None, None, :, None]
    )
    high = lax.reduce_precision(weight, 8, 7)
    low = weight - high

    def spread(v):
        return jnp.where(picks, v, 0.0).astype(BF).reshape(chips, 2 * cap, rows)

    pick = picks.astype(BF).reshape(chips, 2 * cap, rows)
    pick_high = spread(high[:, :, None, :])
    pick_low = spread(low[:, :, None, :])
    row_scale = jnp.sum(jnp.where(picks, metas[:, 3][:, None, None, :], 0.0), -1).reshape(
        chips, 2 * cap
    )
    edge_weight = jnp.sum(jnp.where(picks[-1], weight[-1][:, None, :], 0.0), -1)

    def ordering(d, way):
        source = (chip - d) % chips
        best = jnp.zeros((rows,), jnp.int32)
        for ids in (first[where[d]], second[where[d]]):
            dist = (way * (ids // 2 - source)) % chips
            good = (dist < far) | ((dist == far) & (ids % 2 == (0 if way == 1 else 1)))
            best = jnp.maximum(best, jnp.where(good, dist, 0))
        return best

    combos = [(t if t == far else way * t, way) for t in range(near, far) for way in (1, -1)]
    reach = jnp.stack([ordering(d, way) for d, way in combos])
    levels = jnp.arange(far, near, -1, dtype=jnp.int32)
    at = reach[:, None, :] == levels[None, :, None]
    rank_in = dot(at.astype(BF).reshape(-1, rows), before).reshape(at.shape)
    total = jnp.sum(at.astype(F32), -1)
    base = jnp.cumsum(total, 1) - total
    rank = jnp.sum(jnp.where(at, rank_in + base[:, :, None], 0.0), 1)
    rank = jnp.where(reach > near, rank, -1.0)
    place = (
        rank[:, None, :] == jnp.arange(size[near + 1], dtype=F32)[None, :, None]
    ).astype(BF)

    pieces = [tokens[:, h * part : (h + 1) * part] for h in range(HALVES)]
    gains = [norm_gain[h * part : (h + 1) * part] for h in range(HALVES)]

    def chosen(select, packet, d):
        return [
            (dot(select, packet[h]) * row_scale[where[d]][:, None] * gains[h]).astype(BF)
            for h in range(HALVES)
        ]

    def sorted_picks(t, way):
        i = combos.index((way * t, way))
        w = where[way * t]
        three = jnp.concatenate([pick[w], pick_high[w], pick_low[w]], 0)
        return dot(three, place[i][: size[t]], ((1,), (1,))).astype(BF)

    packet = {1: pieces, -1: pieces}
    picked = {0: [chosen(pick[0], pieces, 0)]}
    backs = {}
    for t in range(1, far + 1):
        for way in (1, -1):
            if t == near + 1:
                i = combos.index((way * near, way))
                packet[way] = [dot(place[i], p).astype(BF) for p in packet[way]]
            packet[way] = [shift(p[: size[t]], way) for p in packet[way]]
        if t < far:
            for way in (1, -1):
                w = where[way * t]
                if t <= near:
                    select = pick[w]
                    backs[t, way] = jnp.concatenate([pick_high[w], pick_low[w]], 0)
                else:
                    three = sorted_picks(t, way)
                    select = three[: 2 * cap]
                    backs[t, way] = three[2 * cap :]
                picked.setdefault(t, []).append(chosen(select, packet[way], way * t))
        else:
            sides = []
            for which in (0, 1):
                s = row_scale[-1][which * cap : (which + 1) * cap, None]
                sides.append(
                    [
                        (
                            jnp.where(core == which, packet[1][h], packet[-1][h]).astype(F32)
                            * s
                            * gains[h]
                        ).astype(BF)
                        for h in range(HALVES)
                    ]
                )
            picked[t] = [[jnp.concatenate([sides[0][h], sides[1][h]], 0) for h in range(HALVES)]]

    groups = [[0, 1, 2], [3, 4], [5, 6], [far - 1, far]]
    done = {}
    for group in groups:
        blocks = [(t, j) for t in group for j in range(len(picked[t]))]
        full = [jnp.concatenate(picked[t][j], 1) for t, j in blocks]
        own = jnp.concatenate([b[:cap] for b in full], 0)
        other = jnp.concatenate([b[cap:] for b in full], 0)
        x = jnp.concatenate([own, swap(other)], 0)
        gate = dot(x, w_gate[0])
        upper = dot(x, w_up[0])
        hidden = (jax.nn.silu(gate) * upper).astype(BF)
        result = dot(hidden, w_down[0]).astype(BF)
        n = len(blocks) * cap
        theirs = swap(result[n:])
        for k, key in enumerate(blocks):
            s = slice(k * cap, (k + 1) * cap)
            done[key] = (result[s], theirs[s])

    def twice(key, h):
        both = jnp.concatenate(done[key], 0)[:, h * part : (h + 1) * part]
        return jnp.concatenate([both, both], 0)

    coming = {1: None, -1: None}
    mine, theirs = done[far, 0]
    mine = (mine.astype(F32) * edge_weight[0][:, None]).astype(BF)
    theirs = (theirs.astype(F32) * edge_weight[1][:, None]).astype(BF)
    for way in (1, -1):
        side = jnp.where(core == (0 if way == 1 else 1), mine, theirs)
        coming[way] = [shift(side[:, h * part : (h + 1) * part], -way) for h in range(HALVES)]
    for t in range(far - 1, 0, -1):
        for way in (1, -1):
            sums = []
            for h in range(HALVES):
                add = dot(backs[t, way], twice((t, 0 if way == 1 else 1), h), ((0,), (0,)))
                got = coming[way][h]
                if t == near:
                    i = combos.index((way * near, way))
                    add = add + dot(place[i], got, ((0,), (0,)))
                else:
                    got = got.astype(F32)
                    add = add + jnp.pad(got, ((0, size[t] - got.shape[0]), (0, 0)))
                sums.append(shift(add.astype(BF), -way))
            coming[way] = sums
    outs = []
    back = jnp.concatenate([pick_high[0], pick_low[0]], 0)
    for h in range(HALVES):
        total = dot(back, twice((0, 0), h), ((0,), (0,)))
        total = total + coming[1][h].astype(F32) + coming[-1][h].astype(F32)
        outs.append(total.astype(BF))
    return jnp.concatenate(outs, 1)


def solution(mesh):
    return jax.shard_map(
        per_device,
        mesh=mesh,
        in_specs=(
            P(("grp", "ep"), None),
            P(),
            P(("grp", "ep"), None),
            P(("grp", "ep"), None),
            P("ep", None, None),
            P("ep", None, None),
            P("ep", None, None),
        ),
        out_specs=P(("grp", "ep"), None),
        check_vma=False,
    )
```

```python
import functools

import jax
import jax.numpy as jnp
from jax import lax
from jax.experimental import pallas as pl
from jax.experimental.pallas import tpu as pltpu
from jax.sharding import PartitionSpec as P


BF = jnp.bfloat16
F32 = jnp.float32
TILE = 256
META = 8
VMEM = pl.BlockSpec(memory_space=pltpu.VMEM)
SMEM = pl.BlockSpec(memory_space=pltpu.SMEM)


def dot(a, b, dims=((1,), (0,))):
    return lax.dot_general(a, b, (dims, ((), ())), preferred_element_type=F32)


def earlier(n):
    row = lax.broadcasted_iota(jnp.int32, (n, n), 0)
    col = lax.broadcasted_iota(jnp.int32, (n, n), 1)
    return (row < col).astype(BF)


def select_kernel(cap, plan, ids, gain, *refs):
    count = sum(len(block) for block in plan)
    packets = refs[: 2 * count]
    own_ref, other_ref = refs[2 * count : 2 * count + 2]
    backs = refs[2 * count + 2 :]
    me = ids[0]
    slots = lax.broadcasted_iota(jnp.int32, (cap, 1), 0).astype(F32)
    triangles, chosen, scales = {}, {}, []
    half = gain.shape[1] // 2
    for block in plan:
        scales.append(jnp.zeros((2 * cap, 1), F32))
        for index, size, side in block:
            meta = packets[2 * index][size : size + META, : max(size, 128)].astype(F32)[:, :size]
            hits = []
            for who in (me, me ^ 1):
                name = (who + 1).astype(F32)
                if side is not None:
                    name = jnp.where(who % 2 == side, name, -1.0)
                hits.append((meta[0:1] == name, meta[1:2] == name))
            marks = [(a | c) for a, c in hits]
            if size not in triangles:
                triangles[size] = earlier(size)
            stacked = jnp.concatenate(
                [m.astype(F32) for m in marks] + [jnp.zeros((META - 2, size), F32)], 0
            )
            before = dot(stacked.astype(BF), triangles[size])
            picks, highs, lows = [], [], []
            for k in (0, 1):
                slot = jnp.where(marks[k], before[k : k + 1], -1.0)
                pick = slots == slot
                a, c = hits[k]
                high = jnp.where(a, meta[2:3], 0.0) + jnp.where(c, meta[4:5], 0.0)
                low = jnp.where(a, meta[3:4], 0.0) + jnp.where(c, meta[5:6], 0.0)
                picks.append(pick.astype(F32))
                highs.append(jnp.where(pick, high, 0.0))
                lows.append(jnp.where(pick, low, 0.0))
            pick = jnp.concatenate(picks, 0)
            backs[index][...] = jnp.concatenate(highs + lows, 0).astype(BF)
            scales[-1] += jnp.sum(pick * (meta[6:7] + meta[7:8]), 1, keepdims=True)
            chosen[index] = pick.astype(BF)

    def columns(j, _):
        start = pl.multiple_of(j * TILE, TILE)
        for h in (0, 1):
            cols = pl.ds(pl.multiple_of(h * half + start, TILE), TILE)
            for b, block in enumerate(plan):
                value = sum(
                    dot(chosen[i], packets[2 * i + h][0:n, pl.ds(start, TILE)]) for i, n, _ in block
                )
                value = (value * scales[b] * gain[0:1, cols]).astype(BF)
                own_ref[b * cap : (b + 1) * cap, cols] = value[:cap]
                other_ref[b * cap : (b + 1) * cap, cols] = value[cap:]
        return 0

    lax.fori_loop(0, half // TILE, columns, 0)


def select(cap, plan, me, gain, packets):
    blocks = len(plan)
    flat = [half for p in packets for half in p]
    width = gain.shape[1]
    sizes = [p[1].shape[0] for p in packets]
    rows = jax.ShapeDtypeStruct((blocks * cap, width), BF)
    flops = sum(2 * 2 * cap * s * (width + s) for s in sizes)
    out = pl.pallas_call(
        functools.partial(select_kernel, cap, plan),
        out_shape=[rows, rows] + [jax.ShapeDtypeStruct((4 * cap, s), BF) for s in sizes],
        in_specs=[SMEM] + [VMEM] * (1 + len(flat)),
        out_specs=[VMEM] * (2 + len(sizes)),
        cost_estimate=pl.CostEstimate(
            flops=flops, bytes_accessed=sum(f.size * 2 for f in flat), transcendentals=0
        ),
        name="select",
    )(me, gain, *flat)
    return out[0], out[1], out[2:]


def compact_kernel(rows, size, chips, way, info, packet, out, place_ref):
    far = chips // 2
    source, near = info[0], info[1]
    meta_bits = packet[rows : rows + META, 0:rows]
    meta = meta_bits.astype(F32)
    best = jnp.zeros((1, rows), jnp.int32)
    for k in (0, 1):
        expert = meta[k : k + 1].astype(jnp.int32) - 1
        gap = way * ((expert >> 1) - source) + 2 * chips
        dist = gap & (chips - 1)
        good = (dist < far) | ((dist == far) & ((expert & 1) == (0 if way == 1 else 1)))
        best = jnp.maximum(best, jnp.where(good, dist, 0))
    level = lax.broadcasted_iota(jnp.int32, (META, 1), 0)
    at = (best == (far - level)) & (best > near)
    ind = at.astype(F32)
    before = dot(ind.astype(BF), earlier(rows))
    count = jnp.sum(ind, 1, keepdims=True)
    rank = jnp.zeros((1, rows), F32)
    base = jnp.zeros((1, 1), F32)
    for l in range(META):
        rank = rank + ind[l : l + 1] * (before[l : l + 1] + base + 1.0)
        base = base + count[l : l + 1]
    slot = lax.broadcasted_iota(jnp.int32, (size, 1), 0).astype(F32) + 1.0
    place = (slot == rank).astype(F32).astype(BF)
    place_ref[...] = place
    out[0:size, :] = dot(place, packet[0:rows, :]).astype(BF)
    moved = dot(meta_bits, place, ((1,), (1,)))
    filler = packet.shape[1] - size
    out[size : size + META, :] = jnp.concatenate(
        [moved, jnp.zeros((META, filler), F32)], 1
    ).astype(BF)


def compact(rows, size, chips, way, info, packet):
    return pl.pallas_call(
        functools.partial(compact_kernel, rows, size, chips, way),
        out_shape=[
            jax.ShapeDtypeStruct((size + META, packet.shape[1]), BF),
            jax.ShapeDtypeStruct((size, rows), BF),
        ],
        in_specs=[SMEM, VMEM],
        out_specs=[VMEM, VMEM],
        cost_estimate=pl.CostEstimate(
            flops=2 * rows * size * packet.shape[1],
            bytes_accessed=4 * packet.size,
            transcendentals=0,
        ),
        name="compact",
    )(info, packet)


def expert_kernel(counts, *refs):
    groups = len(counts)
    inputs = refs[: 2 * groups]
    w_gate, w_up, w_down = refs[2 * groups : 2 * groups + 3]
    own_out, other_out, x, total = refs[2 * groups + 3 :]
    n = sum(counts)
    step = pl.program_id(0)

    @pl.when(step == 0)
    def _():
        at = 0
        for side in (0, 1):
            for g, count in enumerate(counts):
                x[at : at + count, :] = inputs[side * groups + g][...]
                at += count

    gate = dot(x[...], w_gate[0])
    upper = dot(x[...], w_up[0])
    hidden = (gate / (1.0 + jnp.exp(-gate)) * upper).astype(BF)
    piece = dot(hidden, w_down[0])

    @pl.when(step == 0)
    def _():
        total[...] = piece

    @pl.when(step > 0)
    def _():
        total[...] += piece

    @pl.when(step == pl.num_programs(0) - 1)
    def _():
        own_out[...] = total[0:n, :].astype(BF)
        other_out[...] = total[n : 2 * n, :].astype(BF)


def expert(owns, others, w_gate, w_up, w_down):
    counts = [o.shape[0] for o in owns]
    n, width = sum(counts), owns[0].shape[1]
    hidden = w_gate.shape[2]

    def whole(rows):
        return pl.BlockSpec((rows, width), lambda i: (0, 0))

    return pl.pallas_call(
        functools.partial(expert_kernel, counts),
        grid=(hidden // TILE,),
        in_specs=[whole(c) for c in counts + counts]
        + [
            pl.BlockSpec((1, width, TILE), lambda i: (0, 0, i)),
            pl.BlockSpec((1, width, TILE), lambda i: (0, 0, i)),
            pl.BlockSpec((1, TILE, width), lambda i: (0, i, 0)),
        ],
        out_specs=[whole(n), whole(n)],
        out_shape=[jax.ShapeDtypeStruct((n, width), BF)] * 2,
        scratch_shapes=[pltpu.VMEM((2 * n, width), BF), pltpu.VMEM((2 * n, width), F32)],
        cost_estimate=pl.CostEstimate(
            flops=2 * n * 6 * width * hidden,
            bytes_accessed=6 * width * hidden,
            transcendentals=2 * n * hidden,
        ),
        name="expert",
    )(*owns, *others, w_gate, w_up, w_down)


def per_device(tokens, norm_gain, expert_ids, gate_weights, w_gate, w_up, w_down):
    ep = lax.axis_size("ep")
    chips = ep // 2
    far = chips // 2
    rows, width = tokens.shape
    cap = 2 * rows * expert_ids.shape[1] // ep
    size = {t: min(rows, cap * (2 * (far - t) + 1)) for t in range(1, far + 1)}
    near = max(t for t in size if size[t] == rows)
    half = width // 2
    me = lax.axis_index("ep").astype(jnp.int32)
    chip = me // 2
    me_ref = me.reshape(1)
    gain = norm_gain.reshape(1, width)

    def shift(x, hops):
        return lax.ppermute(x, "ep", [(i, (i + 2 * hops) % ep) for i in range(ep)])

    def swap(x):
        return lax.ppermute(x, "ep", [(i, i ^ 1) for i in range(ep)])

    values = tokens.astype(F32)
    scale = lax.rsqrt(jnp.mean(values * values, -1) + 1e-06)[None, :]
    facts = jnp.concatenate([gate_weights.T, scale], 0)
    high = lax.reduce_precision(facts, 8, 7)
    low = facts - high
    names = (expert_ids.T + 1).astype(F32)
    meta = jnp.concatenate(
        [names, high[0:1], low[0:1], high[1:2], low[1:2], high[2:3], low[2:3]], 0
    ).astype(BF)
    meta = jnp.pad(meta, ((0, 0), (0, half - rows)))
    local = (jnp.concatenate([tokens[:, :half], meta], 0), tokens[:, half:])

    packet = {1: local, -1: local}
    places = {}
    arrived = {0: local}
    for t in range(1, far + 1):
        for way in (1, -1):
            first, second = packet[way]
            if t == near + 1:
                info = jnp.stack([(chip - way * near) % chips, jnp.int32(near)])
                first, place = compact(rows, size[t], chips, way, info, first)
                second = dot(place, second).astype(BF)
                places[way] = place
            elif t > near:
                last = size[t - 1]
                first = jnp.concatenate([first[: size[t]], first[last:]], 0)
                second = second[: size[t]]
            sent = []
            for x in (first, second):
                sent.append(shift(x, way))
            packet[way] = tuple(sent)
            arrived[t, way] = packet[way]

    groups = [[0, 1], [2, 3], [4, 5], [6], [far - 1, far]]
    calls = [[0], [1], [2, 3, 4]]
    call_of = {g: k for k, call in enumerate(calls) for g in call}
    results, backs, slot_of = {}, {}, {}
    filled = [0] * len(calls)
    taken = {}
    for g, group in enumerate(groups):
        k = call_of[g]
        packets, plan, keys = [], [], []

        def add(key, sizes):
            packets.append(arrived[key])
            keys.append(key)
            return (len(packets) - 1, sizes, None)

        for t in group:
            if t == 0:
                plan.append((add(0, rows),))
                slot_of[0] = (k, filled[k] + len(plan) - 1)
            elif t < far:
                for way in (1, -1):
                    plan.append((add((t, way), size[t]),))
                    slot_of[t, way] = (k, filled[k] + len(plan) - 1)
            else:
                block = []
                for way in (1, -1):
                    i, s, _ = add((t, way), size[t])
                    block.append((i, s, 0 if way == 1 else 1))
                    slot_of[t, way] = (k, filled[k] + len(plan))
                plan.append(tuple(block))
        own, other, mats = select(cap, tuple(plan), me_ref, gain, packets)
        for key, mat in zip(keys, mats):
            backs[key] = mat
        filled[k] += len(plan)
        taken[g] = (own, swap(other))
    for k, call in enumerate(calls):
        mine, theirs = expert(
            [taken[g][0] for g in call], [taken[g][1] for g in call], w_gate, w_up, w_down
        )
        results[k] = (mine, swap(theirs))

    def found(key, h):
        g, b = slot_of[key]
        cols = slice(h * half, (h + 1) * half)
        both = [r[b * cap : (b + 1) * cap, cols] for r in results[g]]
        return jnp.concatenate(both + both, 0)

    coming = {}
    for t in range(far, 0, -1):
        for way in (1, -1):
            sums = []
            for h in (0, 1):
                add = dot(backs[t, way], found((t, way), h), ((0,), (0,)))
                if t < far:
                    got = coming[way][h]
                    if t == near:
                        add = add + dot(places[way], got, ((0,), (0,)))
                    else:
                        got = got.astype(F32)
                        add = add + jnp.pad(got, ((0, size[t] - got.shape[0]), (0, 0)))
                sums.append(shift(add.astype(BF), -way))
            coming[way] = sums
    outs = []
    for h in (0, 1):
        total = dot(backs[0], found(0, h), ((0,), (0,)))
        total = total + coming[1][h].astype(F32) + coming[-1][h].astype(F32)
        outs.append(total.astype(BF))
    return jnp.concatenate(outs, 1)


def solution(mesh):
    return jax.shard_map(
        per_device,
        mesh=mesh,
        in_specs=(
            P(("grp", "ep"), None),
            P(),
            P(("grp", "ep"), None),
            P(("grp", "ep"), None),
            P("ep", None, None),
            P("ep", None, None),
            P("ep", None, None),
        ),
        out_specs=P(("grp", "ep"), None),
        check_vma=False,
    )
```

```python
import functools

import jax
import jax.numpy as jnp
from jax import lax
from jax.experimental import pallas as pl
from jax.experimental.pallas import tpu as pltpu
from jax.sharding import PartitionSpec as P


BF = jnp.bfloat16
F32 = jnp.float32
TILE = 256
LIMIT = 36 * 2**20
META = 8
VMEM = pl.BlockSpec(memory_space=pltpu.VMEM)
SMEM = pl.BlockSpec(memory_space=pltpu.SMEM)


def dot(a, b, dims=((1,), (0,))):
    return lax.dot_general(a, b, (dims, ((), ())), preferred_element_type=F32)


def earlier(n):
    row = lax.broadcasted_iota(jnp.int32, (n, n), 0)
    col = lax.broadcasted_iota(jnp.int32, (n, n), 1)
    return (row < col).astype(BF)


def select_kernel(cap, plan, ids, gain, *refs):
    count = len(plan)
    packets = refs[:count]
    own_ref = refs[count]
    other_ref = refs[count + 1] if any(both for _, both in plan) else None
    backs = refs[-count:]
    me = ids[0]
    slots = lax.broadcasted_iota(jnp.int32, (cap, 1), 0).astype(F32)
    triangles, chosen, scales = {}, [], []
    for packet, back, (size, both) in zip(packets, backs, plan):
        meta = packet[size : size + META, : max(size, 128)].astype(F32)[:, :size]
        hits = []
        for who in (me, me ^ 1) if both else (me,):
            name = (who + 1).astype(F32)
            hits.append((meta[0:1] == name, meta[1:2] == name))
        marks = [(a | c) for a, c in hits]
        if size not in triangles:
            triangles[size] = earlier(size)
        stacked = jnp.concatenate(
            [m.astype(F32) for m in marks] + [jnp.zeros((META - len(marks), size), F32)], 0
        )
        before = dot(stacked.astype(BF), triangles[size])
        picks, highs, lows = [], [], []
        for k, (a, c) in enumerate(hits):
            slot = jnp.where(marks[k], before[k : k + 1], -1.0)
            pick = slots == slot
            high = jnp.where(a, meta[2:3], 0.0) + jnp.where(c, meta[4:5], 0.0)
            low = jnp.where(a, meta[3:4], 0.0) + jnp.where(c, meta[5:6], 0.0)
            picks.append(pick.astype(F32))
            highs.append(jnp.where(pick, high, 0.0))
            lows.append(jnp.where(pick, low, 0.0))
        pick = jnp.concatenate(picks, 0)
        back[...] = jnp.concatenate(highs + lows, 0).astype(BF)
        scales.append(jnp.sum(pick * (meta[6:7] + meta[7:8]), 1, keepdims=True))
        chosen.append(pick.astype(BF))

    def columns(j, _):
        cols = pl.ds(pl.multiple_of(j * TILE, TILE), TILE)
        twos = 0
        for i, (size, both) in enumerate(plan):
            value = dot(chosen[i], packets[i][0:size, cols])
            value = (value * scales[i] * gain[0:1, cols]).astype(BF)
            own_ref[i * cap : (i + 1) * cap, cols] = value[:cap]
            if both:
                other_ref[twos * cap : (twos + 1) * cap, cols] = value[cap:]
                twos += 1
        return 0

    lax.fori_loop(0, gain.shape[1] // TILE, columns, 0)


def select(cap, plan, me, gain, packets):
    width = gain.shape[1]
    twos = sum(both for _, both in plan)
    outs = [jax.ShapeDtypeStruct((len(plan) * cap, width), BF)]
    if twos:
        outs.append(jax.ShapeDtypeStruct((twos * cap, width), BF))
    outs += [jax.ShapeDtypeStruct(((4 if both else 2) * cap, n), BF) for n, both in plan]
    out = pl.pallas_call(
        functools.partial(select_kernel, cap, plan),
        out_shape=outs,
        in_specs=[SMEM] + [VMEM] * (1 + len(packets)),
        out_specs=[VMEM] * len(outs),
        cost_estimate=pl.CostEstimate(
            flops=sum(4 * cap * n * (width + n) for n, _ in plan),
            bytes_accessed=sum(p.size * 2 for p in packets),
            transcendentals=0,
        ),
        compiler_params=pltpu.CompilerParams(vmem_limit_bytes=LIMIT),
        name="select",
    )(me, gain, *packets)
    return out[0], (out[1] if twos else None), out[len(outs) - len(plan) :]


def compact_kernel(rows, size, chips, info, packet, out, place_ref):
    far = chips // 2
    source, near, way, core = info[0], info[1], info[2], info[3]
    meta_bits = packet[rows : rows + META, 0:rows]
    meta = meta_bits.astype(F32)
    best = jnp.zeros((1, rows), jnp.int32)
    for k in (0, 1):
        expert = meta[k : k + 1].astype(jnp.int32) - 1
        dist = (way * ((expert >> 1) - source) + 2 * chips) & (chips - 1)
        good = (dist < far) | ((dist == far) & ((expert & 1) == core))
        best = jnp.maximum(best, jnp.where(good, dist, 0))
    level = lax.broadcasted_iota(jnp.int32, (META, 1), 0)
    at = (best == (far - level)) & (best > near)
    ind = at.astype(F32)
    before = dot(ind.astype(BF), earlier(rows))
    count = jnp.sum(ind, 1, keepdims=True)
    rank = jnp.zeros((1, rows), F32)
    base = jnp.zeros((1, 1), F32)
    for l in range(META):
        rank = rank + ind[l : l + 1] * (before[l : l + 1] + base + 1.0)
        base = base + count[l : l + 1]
    slot = lax.broadcasted_iota(jnp.int32, (size, 1), 0).astype(F32) + 1.0
    place = (slot == rank).astype(F32).astype(BF)
    place_ref[...] = place

    def columns(j, _):
        cols = pl.ds(pl.multiple_of(j * TILE, TILE), TILE)
        out[0:size, cols] = dot(place, packet[0:rows, cols]).astype(BF)
        return 0

    lax.fori_loop(0, packet.shape[1] // TILE, columns, 0)
    moved = dot(meta_bits, place, ((1,), (1,)))
    filler = packet.shape[1] - size
    out[size : size + META, :] = jnp.concatenate(
        [moved, jnp.zeros((META, filler), F32)], 1
    ).astype(BF)


def compact(rows, size, chips, info, packet):
    return pl.pallas_call(
        functools.partial(compact_kernel, rows, size, chips),
        out_shape=[
            jax.ShapeDtypeStruct((size + META, packet.shape[1]), BF),
            jax.ShapeDtypeStruct((size, rows), BF),
        ],
        in_specs=[SMEM, VMEM],
        out_specs=[VMEM, VMEM],
        cost_estimate=pl.CostEstimate(
            flops=2 * rows * size * packet.shape[1],
            bytes_accessed=4 * packet.size,
            transcendentals=0,
        ),
        compiler_params=pltpu.CompilerParams(vmem_limit_bytes=LIMIT),
        name="compact",
    )(info, packet)


def expert_kernel(counts, outs, *refs):
    inputs = refs[: len(counts)]
    w_gate, w_up, w_down = refs[len(counts) : len(counts) + 3]
    x, total = refs[-2:]
    at = 0
    for ref, count in zip(inputs, counts):
        x[at : at + count, :] = ref[...]
        at += count

    def piece(j):
        cols = pl.ds(pl.multiple_of(j * TILE, TILE), TILE)
        gate = dot(x[...], w_gate[0, :, cols])
        upper = dot(x[...], w_up[0, :, cols])
        hidden = (gate / (1.0 + jnp.exp(-gate)) * upper).astype(BF)
        return dot(hidden, w_down[0, cols, :])

    total[...] = piece(0)

    def more(j, _):
        total[...] += piece(j)
        return 0

    lax.fori_loop(1, w_gate.shape[2] // TILE, more, 0)
    at = 0
    for ref, count in zip(refs[len(counts) + 3 : -2], outs):
        ref[...] = total[at : at + count, :].astype(BF)
        at += count


def expert(owns, others, w_gate, w_up, w_down):
    counts = [o.shape[0] for o in owns + others]
    outs = [sum(o.shape[0] for o in side) for side in (owns, others) if side]
    n, width = sum(counts), owns[0].shape[1]
    hidden = w_gate.shape[2]
    return pl.pallas_call(
        functools.partial(expert_kernel, counts, outs),
        in_specs=[VMEM] * (len(counts) + 3),
        out_specs=[VMEM] * len(outs),
        out_shape=[jax.ShapeDtypeStruct((m, width), BF) for m in outs],
        scratch_shapes=[pltpu.VMEM((n, width), BF), pltpu.VMEM((n, width), F32)],
        cost_estimate=pl.CostEstimate(
            flops=n * 6 * width * hidden,
            bytes_accessed=6 * width * hidden,
            transcendentals=n * hidden,
        ),
        compiler_params=pltpu.CompilerParams(vmem_limit_bytes=LIMIT),
        name="expert",
    )(*owns, *others, w_gate, w_up, w_down)


def per_device(tokens, norm_gain, expert_ids, gate_weights, w_gate, w_up, w_down):
    ep = lax.axis_size("ep")
    chips = ep // 2
    far = chips // 2
    rows, width = tokens.shape
    cap = 2 * rows * expert_ids.shape[1] // ep
    size = {t: min(rows, cap * (2 * (far - t) + 1)) for t in range(1, far + 1)}
    near = max(t for t in size if size[t] == rows)
    me = lax.axis_index("ep").astype(jnp.int32)
    chip, core = me // 2, me % 2
    me_ref = me.reshape(1)
    gain = norm_gain.reshape(1, width)

    def shift(x, hops):
        return lax.ppermute(
            x,
            "ep",
            [(i, (i + 2 * hops * (1 if i % 2 == 0 else -1)) % ep) for i in range(ep)],
        )

    def swap(x):
        return lax.ppermute(x, "ep", [(i, i ^ 1) for i in range(ep)])

    values = tokens.astype(F32)
    scale = lax.rsqrt(jnp.mean(values * values, -1) + 1e-06)[None, :]
    facts = jnp.concatenate([gate_weights.T, scale], 0)
    high = lax.reduce_precision(facts, 8, 7)
    low = facts - high
    names = (expert_ids.T + 1).astype(F32)
    meta = jnp.concatenate(
        [names, high[0:1], low[0:1], high[1:2], low[1:2], high[2:3], low[2:3]], 0
    ).astype(BF)
    local = jnp.concatenate([tokens, jnp.pad(meta, ((0, 0), (0, width - rows)))], 0)
    packet = [local, swap(local)]

    way = 1 - 2 * core
    info = jnp.stack([(chip - way * near) % chips, jnp.int32(near), way, core])
    places = {}
    arrived = {(0, 0): local}
    for t in range(1, far + 1):
        for q in (0, 1):
            x = packet[q]
            if t == near + 1:
                x, places[q] = compact(rows, size[t], chips, info, x)
            elif t > near:
                x = jnp.concatenate([x[: size[t]], x[size[t - 1] :]], 0)
            packet[q] = shift(x, 1)
            arrived[t, q] = packet[q]

    groups = [[0, 1], [2, 3], [4], [5, 6], [far - 1], [far]]
    calls = {"ffn0": [0], "ffn1": [1, 2], "ffn2": [3, 4], "ffn3": [5]}
    backs, taken, results = {}, {}, {}
    for g, group in enumerate(groups):
        keys = [(t, q) for t in group for q in ((0, 1) if t else (0,))]
        plan = tuple((arrived[key].shape[0] - META, key[0] < far) for key in keys)
        own, other, mats = select(cap, plan, me_ref, gain, [arrived[key] for key in keys])
        for key, mat in zip(keys, mats):
            backs[key] = mat
        if other is not None:
            other = swap(other)
        taken[g] = (keys, own, other)
    for call in calls.values():
        done = expert(
            [taken[g][1] for g in call],
            [taken[g][2] for g in call if taken[g][2] is not None],
            w_gate,
            w_up,
            w_down,
        )
        if len(done) > 1:
            done = [done[0], swap(done[1])]
        for i, key in enumerate(key for g in call for key in taken[g][0]):
            pieces = [r[i * cap : (i + 1) * cap] for r in done]
            results[key] = jnp.concatenate(pieces + pieces, 0)

    coming = {}
    for t in range(far, 0, -1):
        for q in (1, 0):
            add = dot(backs[t, q], results[t, q], ((0,), (0,)))
            if t < far:
                got = coming[q]
                if t == near:
                    add = add + dot(places[q], got, ((0,), (0,)))
                else:
                    got = got.astype(F32)
                    add = add + jnp.pad(got, ((0, size[t] - got.shape[0]), (0, 0)))
            coming[q] = shift(add.astype(BF), -1)
    other_way = swap(coming[1])
    total = dot(backs[0, 0], results[0, 0], ((0,), (0,)))
    total = total + coming[0].astype(F32) + other_way.astype(F32)
    return total.astype(BF)


def solution(mesh):
    return jax.shard_map(
        per_device,
        mesh=mesh,
        in_specs=(
            P(("grp", "ep"), None),
            P(),
            P(("grp", "ep"), None),
            P(("grp", "ep"), None),
            P("ep", None, None),
            P("ep", None, None),
            P("ep", None, None),
        ),
        out_specs=P(("grp", "ep"), None),
        check_vma=False,
    )
```
